256 devices in a mesh: fs: 16 (over y, x), tp: 16 (over z, core).
Axes of the slice: x: 4, y: 4, z: 8, core: 2. Of those that a mesh axis runs over, the one named last changes fastest.
Arguments:
- tokens: bfloat16 [32768, 2048], P(('fs', 'tp')), may hold values from -6 to 6
- norm_gain: float32 [2048], replicated, may hold values from 0.1 to 1.9
- gate_weight: bfloat16 [2048, 5632], P('fs', 'tp'), may hold values from -0.125 to 0.125
- up_weight: bfloat16 [2048, 5632], P('fs', 'tp'), may hold values from -0.125 to 0.125
- down_weight: bfloat16 [5632, 2048], P('tp', 'fs'), may hold values from -0.078125 to 0.078125
Outputs:
- mixed: bfloat16 [32768, 2048], P(('fs', 'tp'))
The draws below stay inside these ranges and needn't reach their ends.
All inputs are finite; a program needn't handle non-finite values.
Results may differ from the reference program's by a relative error of at most 0.0065.
Values may be sent and summed in bfloat16 or wider, within the bound.
A program may use at most 128 MiB of HBM per device.

```python
import jax
import jax.numpy as jnp
from jax import lax

D = 2048
FF = 5632
TOK_DEV = 128
TOKENS = 32768


def shard_levels(stream_key, extent, pieces, low, high):
    factor_of = 1.0
    for dim, blocks in pieces:
        draws = jax.random.uniform(jax.random.fold_in(jax.random.fold_in(stream_key, 6), dim), (blocks,), jnp.float32, low / len(pieces), high / len(pieces))
        factor_of = factor_of * jnp.repeat(jnp.exp(draws), extent[dim] // blocks).reshape((-1,) + (1,) * (len(extent) - 1 - dim))
    return factor_of


def centred(key, dims, scale, limit, cuts=(), held_as=jnp.bfloat16):
    loudness = shard_levels(key, dims, cuts, -0.22, 0.18) if cuts else 1.0
    entries = jax.random.normal(key, dims, jnp.float32) * scale * loudness
    return jnp.minimum(jnp.maximum(entries, -limit), limit).astype(held_as)


def setup_inputs(seed: int = 0) -> dict:
    streams_of = jax.random.split(jax.random.key(seed), 6)
    return {
        "tokens": centred(streams_of[0], (TOKENS, D), 1.0, 6.0, ((0, 256),)),
        "norm_gain": jnp.clip(1.0 + 0.18 * jax.random.normal(streams_of[1], (D,), jnp.float32), 0.1, 1.9),
        "gate_weight": centred(streams_of[2], (D, FF), D ** -0.5, 0.125, ((0, 16), (1, 16))),
        "up_weight": centred(streams_of[3], (D, FF), D ** -0.5, 0.125, ((0, 16), (1, 16))),
        "down_weight": centred(streams_of[4], (FF, D), FF ** -0.5, 0.078125, ((0, 16), (1, 16))),
    }


eps_floor = 0.05

def reference(tokens, norm_gain, gate_weight, up_weight, down_weight):
    blocks = tokens.reshape(-1, TOK_DEV, D)

    def one_block(rows):
        values = rows.astype(jnp.float32)
        factor = lax.rsqrt(lax.optimization_barrier(jnp.mean(values * values, axis=-1, keepdims=True)) + eps_floor)
        normed = (values * factor * norm_gain).astype(jnp.bfloat16)
        gate = jnp.dot(normed, gate_weight, preferred_element_type=jnp.float32)
        upper = jnp.dot(normed, up_weight, preferred_element_type=jnp.float32)
        hidden = (jax.nn.silu(gate) * upper).astype(jnp.bfloat16)
        return jnp.dot(hidden, down_weight, preferred_element_type=jnp.float32).astype(jnp.bfloat16)
    return lax.map(one_block, blocks).reshape(TOKENS, D)
```

```python
import jax
import jax.numpy as jnp
from jax import lax
from jax.experimental import pallas as pl
from jax.experimental.pallas import tpu as pltpu
from jax.sharding import PartitionSpec as P

eps_floor = 0.05
MESH = pl.DeviceIdType.MESH
F32 = jnp.float32
BF16 = jnp.bfloat16

SIDE, Z = 4, 8
ROWS, D, H = 128, 2048, 352
HALF = ROWS // 2
SLOTS = SIDE * SIDE
PAIRS = SLOTS // 2
UNITS = ((0, 0), (1, 0), (0, 1), (1, 1), (2, 0), (2, 1))
OWN, DOWN1, UP1, DOWN2, UP2 = 0, ROWS, 2 * ROWS, 3 * ROWS, 3 * ROWS + HALF
M = 4 * ROWS
SPAN = ((0, ROWS, -1), (ROWS, ROWS, 1), (2 * ROWS, HALF, -2), (2 * ROWS + HALF, HALF, 2))
WIDE = 2 * H
TILES = tuple((n, min(n + 256, WIDE)) for n in range(0, WIDE, 256))


def kernel(tok, gain, gw, uw, dw, out, T, W, G, hid, part, S, R,
           local, w_send, w_recv, s_send, s_recv, x_send, x_recv, t_send, t_recv, q_send, q_recv):
    f, t = lax.axis_index("fs"), lax.axis_index("tp")
    y, x, z, c = f // SIDE, f % SIDE, t // 2, t % 2

    def fs_at(j, i, core=c):
        dy = jnp.where(core == 0, j, i)
        dx = jnp.where(core == 0, i, j)
        return lax.rem(y + dy, SIDE) * SIDE + lax.rem(x + dx, SIDE)

    def z_at(dz):
        return {"tp": lax.rem(z + dz + Z, Z) * 2 + c}

    sib = {"tp": z * 2 + 1 - c}

    barrier = pltpu.get_barrier_semaphore()
    peers = [{"fs": fs_at(j, i)} for j, i in ((0, 1), (0, 3), (1, 0), (3, 0), (0, 2))]
    peers += [z_at(dz) for dz in (1, -1, 2, -2, 4)] + [sib]
    for peer in peers:
        pl.semaphore_signal(barrier, inc=1, device_id=peer, device_id_type=MESH)

    def piece(m, p, fs, core):
        return W.at[m, fs // 2, p, pl.ds(pl.multiple_of(core * H, 32), H),
                    pl.ds(pl.multiple_of((fs % 2) * 128, 128), 128)]

    own = [pltpu.make_async_copy(ref, piece(m, 0, f, c), local.at[m]) for m, ref in enumerate((gw, uw, dw))]
    for cp in own:
        cp.start()
    values = tok[...].astype(F32)
    factor = lax.rsqrt(jnp.mean(values * values, axis=-1, keepdims=True) + eps_floor)
    T[OWN:OWN + ROWS] = (values * factor * gain[...]).astype(BF16)
    pl.semaphore_wait(barrier, len(peers))
    for cp in own:
        cp.wait()

    sent = []

    def send(src, dst, send_sem, recv_sem, device):
        cp = pltpu.make_async_remote_copy(src_ref=src, dst_ref=dst, send_sem=send_sem, recv_sem=recv_sem,
                                          device_id=device, device_id_type=MESH)
        cp.start()
        sent.append(cp)

    def landed(ref, sem):
        pltpu.make_async_copy(ref, ref, sem).wait()

    count = [0]

    def hop(u, j, i, dj, di):
        m, p = UNITS[u]
        ref = piece(m, p, fs_at(j, i), c)
        slot = ((j - dj) % SIDE) * SIDE + (i - di) % SIDE
        send(ref, ref, w_send.at[count[0]], w_recv.at[u, slot], {"fs": fs_at(dj, di)})
        count[0] += 1

    def to_sib(u, j, i):
        m, p = UNITS[u]
        ref = piece(m, p, fs_at(j, i), c)
        k = j * SIDE + i
        send(ref, ref, s_send.at[u, k], s_recv.at[u, k], sib)

    def from_sib(u, j, i):
        m, p = UNITS[u]
        landed(piece(m, p, fs_at(j, i, 1 - c), 1 - c), s_recv.at[u, j * SIDE + i])

    def arrive(u, j, i):
        m, p = UNITS[u]
        landed(piece(m, p, fs_at(j, i), c), w_recv.at[u, j * SIDE + i])

    def exchange(m):
        send(piece(m, 0, f, c), piece(m, 1, f, c), x_send.at[m], x_recv.at[m], z_at(4))

    def begin(u):
        m, p = UNITS[u]
        if p == 1:
            landed(piece(m, 1, f, c), x_recv.at[m])
        for di in (1, 3, 2):
            hop(u, 0, 0, 0, di)
        for dj in (1, 3):
            hop(u, 0, 0, dj, 0)
        to_sib(u, 0, 0)

    def spread(u, i):
        arrive(u, 0, i)
        hop(u, 0, i, 1, 0)
        hop(u, 0, i, 3, 0)
        to_sib(u, 0, i)

    def relay(u, i):
        for j in ((3, 1) if i % 2 == 0 else (1, 3)):
            arrive(u, j, i)
            if i % 2 == 0 and j == 3:
                hop(u, 3, i, 1, 0)
            if i % 2 == 1 and j == 1:
                hop(u, 1, i, 3, 0)
            to_sib(u, j, i)

    def finish(u, i):
        arrive(u, 2, i)
        to_sib(u, 2, i)

    order = (0, 1, 3, 2)

    def tok_send(k, src, dst, dz):
        send(T.at[src:src + HALF], T.at[dst:dst + HALF], t_send.at[k], t_recv.at[k], z_at(dz))

    def tok_wait(k, dst):
        landed(T.at[dst:dst + HALF], t_recv.at[k])

    def all_sib(u):
        for j in range(SIDE):
            for i in range(SIDE):
                from_sib(u, j, i)

    def wide_dot(m, p, n0, n1):
        total = None
        for q in range(PAIRS):
            d = lax.dot_general(T[:, q * 256:(q + 1) * 256], W[m, q, p, n0:n1, :],
                                (((1,), (1,)), ((), ())), preferred_element_type=F32)
            total = d if total is None else total + d
        return total

    def gate(p):
        for n0, n1 in TILES:
            G[:, n0:n1] = wide_dot(0, p, n0, n1)

    def up(p):
        for n0, n1 in TILES:
            hid[p, :, n0:n1] = (jax.nn.silu(G[:, n0:n1]) * wide_dot(1, p, n0, n1)).astype(BF16)

    def pair_of(oy, px):
        return lax.rem(y + oy, SIDE) * 2 + px

    def down(oy):
        @pl.loop(0, 2)
        def _(px):
            q = pair_of(oy, px)
            total = None
            for p in range(2):
                d = jnp.dot(hid[p], W[2, q, p], preferred_element_type=F32)
                total = d if total is None else total + d
            part[q] = total[:ROWS]
            S[q] = total[ROWS:].astype(BF16)
            for k, (r0, n, dz) in enumerate(SPAN):
                pltpu.make_async_remote_copy(
                    src_ref=S.at[q, r0:r0 + n], dst_ref=R.at[q, r0:r0 + n],
                    send_sem=q_send.at[oy, px, k], recv_sem=q_recv.at[oy, px, k],
                    device_id=z_at(dz), device_id_type=MESH).start()

    def total_of(oy):
        @pl.loop(0, 2)
        def _(px):
            q = pair_of(oy, px)
            for k, (r0, n, dz) in enumerate(SPAN):
                landed(R.at[q, r0:r0 + n], q_recv.at[oy, px, k])
            for h in range(2):
                a = h * HALF
                total = part[q, a:a + HALF] + R[q, a:a + HALF].astype(F32)
                total = total + R[q, ROWS + a:ROWS + a + HALF].astype(F32)
                total = total + R[q, 2 * ROWS + a:2 * ROWS + a + HALF].astype(F32)
                out[a:a + HALF, pl.ds(pl.multiple_of(q * 256, 256), 256)] = total.astype(BF16)

    begin(0)
    exchange(0)
    tok_send(0, OWN, DOWN1, 1)
    tok_send(1, OWN + HALF, UP1 + HALF, -1)
    exchange(1)
    tok_send(2, OWN + HALF, DOWN1 + HALF, 1)
    tok_send(3, OWN, UP1, -1)
    begin(1)
    for i in (1, 3, 2):
        spread(0, i)
    begin(2)
    for i in (1, 3, 2):
        spread(1, i)
    for i in order:
        relay(0, i)
    tok_wait(0, DOWN1)
    tok_send(4, DOWN1, DOWN2, 1)
    tok_wait(1, UP1 + HALF)
    tok_send(5, UP1 + HALF, UP2, -1)
    exchange(2)
    begin(3)
    for i in (1, 3, 2):
        spread(2, i)
    for i in order:
        relay(1, i)
    for i in order:
        finish(0, i)
    begin(4)
    for i in (1, 3, 2):
        spread(3, i)
    for i in order:
        relay(2, i)
    for i in order:
        finish(1, i)
    begin(5)
    tok_wait(2, DOWN1 + HALF)
    tok_wait(3, UP1)
    tok_wait(4, DOWN2)
    tok_wait(5, UP2)
    all_sib(0)
    gate(0)
    for i in (1, 3, 2):
        spread(4, i)
        spread(5, i)
    for i in order:
        relay(3, i)
    all_sib(1)
    up(0)
    for i in order:
        finish(2, i)
    for u in (4, 5):
        relay(u, 0)
    all_sib(2)
    gate(1)
    for i in order:
        finish(3, i)
    for u in (4, 5):
        relay(u, 1)
    all_sib(3)
    up(1)
    for u in (4, 5):
        finish(u, 0)
    for u in (4, 5):
        for j, i in [(0, n) for n in range(SIDE)] + [(n, 0) for n in range(1, SIDE)]:
            from_sib(u, j, i)
    down(0)
    for i in (3, 2):
        for u in (4, 5):
            relay(u, i)
    for u in (4, 5):
        finish(u, 1)
    for u in (4, 5):
        for j, i in ((1, 1), (1, 2), (1, 3), (2, 1), (3, 1)):
            from_sib(u, j, i)
    down(1)
    for u in (4, 5):
        finish(u, 3)
    for u in (4, 5):
        for j, i in ((3, 3), (2, 3), (3, 2)):
            from_sib(u, j, i)
    down(3)
    for u in (4, 5):
        finish(u, 2)
    for u in (4, 5):
        from_sib(u, 2, 2)
    down(2)
    for oy in order:
        total_of(oy)

    for cp in sent:
        cp.wait_send()

    @pl.loop(0, PAIRS)
    def _(n):
        oy, px = n // 2, n % 2
        for k, (r0, rows, dz) in enumerate(SPAN):
            ref = S.at[pair_of(oy, px), r0:r0 + rows]
            pltpu.make_async_copy(ref, ref, q_send.at[oy, px, k]).wait()


def layer(tokens, norm_gain, gate_weight, up_weight, down_weight):
    vmem = pl.BlockSpec(memory_space=pltpu.VMEM)
    hbm = pl.BlockSpec(memory_space=pl.ANY)
    dma = pltpu.SemaphoreType.DMA
    n_hops = len(UNITS) * (SLOTS - 1)
    return pl.pallas_call(
        kernel,
        out_shape=pltpu.VMEM((ROWS, D), BF16),
        in_specs=[vmem] * 2 + [hbm] * 3,
        out_specs=vmem,
        scratch_shapes=[
            pltpu.VMEM((M, D), BF16),
            pltpu.VMEM((3, PAIRS, 2, WIDE, 256), BF16),
            pltpu.VMEM((M, WIDE), F32),
            pltpu.VMEM((2, M, WIDE), BF16),
            pltpu.VMEM((PAIRS, ROWS, 256), F32),
            pltpu.VMEM((PAIRS, M - ROWS, 256), BF16),
            pltpu.VMEM((PAIRS, M - ROWS, 256), BF16),
            dma((3,)),
            dma((n_hops,)), dma((len(UNITS), SLOTS)),
            dma((len(UNITS), SLOTS)), dma((len(UNITS), SLOTS)),
            dma((3,)), dma((3,)),
            dma((6,)), dma((6,)),
            dma((SIDE, 2, 4)), dma((SIDE, 2, 4)),
        ],
        compiler_params=pltpu.CompilerParams(
            collective_id=0, has_side_effects=True, vmem_limit_bytes=60 * 1024 * 1024),
    )(tokens, norm_gain.reshape(1, D), gate_weight.T, up_weight.T, down_weight)


def solution(mesh):
    return jax.shard_map(
        layer,
        mesh=mesh,
        in_specs=(P(("fs", "tp"), None), P(), P("fs", "tp"), P("fs", "tp"), P("tp", "fs")),
        out_specs=P(("fs", "tp"), None),
        check_vma=False,
    )
```

```python
import jax
import jax.numpy as jnp
from jax import lax
from jax.experimental import pallas as pl
from jax.experimental.pallas import tpu as pltpu
from jax.sharding import PartitionSpec as P

eps_floor = 0.05
MESH = pl.DeviceIdType.MESH
F32 = jnp.float32
BF16 = jnp.bfloat16

SIDE, Z = 4, 8
ROWS, D, H = 128, 2048, 352
HALF = ROWS // 2
SLOTS = SIDE * SIDE
PAIRS = SLOTS // 2
UNITS = ((0, 0), (1, 0), (0, 1), (1, 1), (2, 0), (2, 1))
OWN, DOWN1, UP1, DOWN2, UP2 = 0, ROWS, 2 * ROWS, 3 * ROWS, 3 * ROWS + HALF
M = 4 * ROWS
FIRST = ((0, -1, DOWN2), (1, -1, DOWN1 + HALF), (3, 1, UP2), (4, 1, UP1))
SECOND = ((2, -1, 0, ROWS), (5, 1, 3, ROWS + HALF))
WIDE = 2 * H
STEPS = ((0, 0), (0, 1), (1, 0), (3, 0), (2, 0), (1, 1), (3, 1), (2, 1))
NEEDS = {0: ((0, 0), (0, 1), (0, 3), (1, 0), (3, 0)), 1: ((0, 2), (2, 0)), 2: ((1, 1), (1, 3), (3, 1)), 3: ((3, 3),),
         4: ((2, 1), (2, 3), (1, 2), (3, 2)), 7: ((2, 2),)}
SET_OF = {piece: step for step, pieces in NEEDS.items() for piece in pieces}
TILES = tuple((n, min(n + 256, WIDE)) for n in range(0, WIDE, 256))


def kernel(tok, gain, gw, uw, dw, out, raw, T, W, G, hid, part, S, R,
           local, w_send, w_recv, s_send, s_recv, x_send, x_recv, t_send, t_recv, q_send, q_recv):
    f, t = lax.axis_index("fs"), lax.axis_index("tp")
    y, x, z, c = f // SIDE, f % SIDE, t // 2, t % 2

    def fs_at(j, i, core=c):
        dy = jnp.where(core == 0, j, i)
        dx = jnp.where(core == 0, i, j)
        return lax.rem(y + dy, SIDE) * SIDE + lax.rem(x + dx, SIDE)

    def z_at(dz):
        return {"tp": lax.rem(z + dz + Z, Z) * 2 + c}

    sib = {"tp": z * 2 + 1 - c}

    barrier = pltpu.get_barrier_semaphore()
    peers = [{"fs": fs_at(j, i)} for j, i in ((0, 1), (0, 3), (1, 0), (3, 0), (0, 2))]
    peers += [z_at(dz) for dz in (1, -1, 4)] + [sib]
    for peer in peers:
        pl.semaphore_signal(barrier, inc=1, device_id=peer, device_id_type=MESH)

    def piece(m, p, fs, core):
        return W.at[m, fs // 2, p, pl.ds(pl.multiple_of(core * H, 32), H),
                    pl.ds(pl.multiple_of((fs % 2) * 128, 128), 128)]

    own = [pltpu.make_async_copy(ref, piece(m, 0, f, c), local.at[m]) for m, ref in enumerate((gw, uw, dw))]
    raw_copy = pltpu.make_async_copy(tok, raw, local.at[3])
    for cp in own:
        cp.start()
    raw_copy.start()
    pl.semaphore_wait(barrier, len(peers))
    for cp in own:
        cp.wait()

    def send(src, dst, send_sem, recv_sem, device):
        cp = pltpu.make_async_remote_copy(src_ref=src, dst_ref=dst, send_sem=send_sem, recv_sem=recv_sem,
                                          device_id=device, device_id_type=MESH)
        cp.start()

    def landed(ref, sem):
        pltpu.make_async_copy(ref, ref, sem).wait()

    def hop(u, j, i, dj, di):
        m, p = UNITS[u]
        ref = piece(m, p, fs_at(j, i), c)
        slot = ((j - dj) % SIDE) * SIDE + (i - di) % SIDE
        send(ref, ref, w_send.at[u], w_recv.at[u, slot], {"fs": fs_at(dj, di)})

    def to_sib(u, j, i):
        m, p = UNITS[u]
        ref = piece(m, p, fs_at(j, i), c)
        k = u if u < 4 else 4 + SET_OF[j, i]
        send(ref, ref, s_send.at[u], s_recv.at[k], sib)

    def half_of(core):
        return pl.ds(pl.multiple_of(core * H, 32), H)

    def all_sib(u):
        m, p = UNITS[u]
        landed(W.at[m, :, p, half_of(1 - c), :], s_recv.at[u])

    def set_sib(step):
        landed(W.at[2, 0:len(NEEDS[step]), :, half_of(1 - c), 0:128], s_recv.at[4 + step])

    def arrive(u, j, i):
        m, p = UNITS[u]
        landed(piece(m, p, fs_at(j, i), c), w_recv.at[u, j * SIDE + i])

    def exchange(m):
        send(piece(m, 0, f, c), piece(m, 1, f, c), x_send, x_recv.at[m], z_at(4))

    def begin(u):
        m, p = UNITS[u]
        if p == 1:
            landed(piece(m, 1, f, c), x_recv.at[m])
        for di in (1, 3, 2):
            hop(u, 0, 0, 0, di)
        for dj in (1, 3):
            hop(u, 0, 0, dj, 0)
        to_sib(u, 0, 0)

    def spread(u, i):
        arrive(u, 0, i)
        hop(u, 0, i, 1, 0)
        hop(u, 0, i, 3, 0)
        to_sib(u, 0, i)

    def relay(u, i):
        for j in ((3, 1) if i % 2 == 0 else (1, 3)):
            arrive(u, j, i)
            if i % 2 == 0 and j == 3:
                hop(u, 3, i, 1, 0)
            if i % 2 == 1 and j == 1:
                hop(u, 1, i, 3, 0)
            to_sib(u, j, i)

    def finish(u, i):
        arrive(u, 2, i)
        to_sib(u, 2, i)

    order = (0, 1, 3, 2)

    def tok_send(k, src, dst, dz):
        send(T.at[src:src + HALF], T.at[dst:dst + HALF], t_send, t_recv.at[k], z_at(dz))

    def tok_wait(k, dst):
        landed(T.at[dst:dst + HALF], t_recv.at[k])

    def wide_dot(m, p, n0, n1):
        total = None
        for q in range(PAIRS):
            d = lax.dot_general(T[:, q * 256:(q + 1) * 256], W[m, q, p, n0:n1, :],
                                (((1,), (1,)), ((), ())), preferred_element_type=F32)
            total = d if total is None else total + d
        return total

    def gate(p):
        for n0, n1 in TILES:
            G[:, n0:n1] = wide_dot(0, p, n0, n1)

    def up(p):
        for n0, n1 in TILES:
            hid[p, :, n0:n1] = (jax.nn.silu(G[:, n0:n1]) * wide_dot(1, p, n0, n1)).astype(BF16)

    def pair_of(step):
        dy, far = STEPS[step]
        px = x // 2
        return lax.rem(y + dy, SIDE) * 2 + (1 - px if far else px)

    def sum_send(step, k, dz):
        q = pair_of(step)
        lot = (0, 2, 2, 1, 2, 2)[k]
        send(S.at[q, k], R.at[q, k], q_send, q_recv.at[step, lot], z_at(dz))

    def down(step):
        q = pair_of(step)
        total = None
        for p in range(2):
            d = jnp.dot(hid[p], W[2, q, p], preferred_element_type=F32)
            total = d if total is None else total + d
        part[q, :ROWS] = total[:ROWS]
        part[q, ROWS:ROWS + HALF] = total[DOWN1:DOWN1 + HALF]
        part[q, ROWS + HALF:] = total[UP1 + HALF:UP1 + ROWS]
        for k, dz, r0 in FIRST:
            S[q, k] = total[r0:r0 + HALF].astype(BF16)
            sum_send(step, k, dz)

    def pass_on(step):
        q = pair_of(step)
        for lot, (k, dz, source, r0) in enumerate(SECOND):
            landed(R.at[q, source], q_recv.at[step, lot])
            S[q, k] = (part[q, r0:r0 + HALF] + R[q, source].astype(F32)).astype(BF16)
            sum_send(step, k, dz)

    def total_of(step):
        q = pair_of(step)
        landed(R.at[q, 0:4], q_recv.at[step, 2])
        for a, first, second in ((0, 4, 2), (HALF, 1, 5)):
            total = part[q, a:a + HALF] + R[q, first].astype(F32) + R[q, second].astype(F32)
            out[a:a + HALF, pl.ds(pl.multiple_of(q * 256, 256), 256)] = total.astype(BF16)

    begin(0)
    exchange(0)
    begin(1)
    exchange(1)
    raw_copy.wait()
    values = raw[...].astype(F32)
    factor = lax.rsqrt(jnp.mean(values * values, axis=-1, keepdims=True) + eps_floor)
    T[OWN:OWN + ROWS] = (values * factor * gain[...]).astype(BF16)
    for i in (1, 3, 2):
        spread(0, i)
    tok_send(0, OWN, DOWN1, 1)
    tok_send(1, OWN + HALF, UP1 + HALF, -1)
    tok_send(2, OWN + HALF, DOWN1 + HALF, 1)
    tok_send(3, OWN, UP1, -1)
    begin(2)
    for i in (1, 3, 2):
        spread(1, i)
    for i in order:
        relay(0, i)
    tok_wait(0, DOWN1)
    tok_send(4, DOWN1, DOWN2, 1)
    tok_wait(1, UP1 + HALF)
    tok_send(5, UP1 + HALF, UP2, -1)
    exchange(2)
    begin(3)
    for i in (1, 3, 2):
        spread(2, i)
    for i in order:
        relay(1, i)
    for i in order:
        finish(0, i)
    for i in (1, 3, 2):
        spread(3, i)
    begin(4)
    for i in order:
        relay(2, i)
    for i in order:
        finish(1, i)
    tok_wait(2, DOWN1 + HALF)
    tok_wait(3, UP1)
    tok_wait(4, DOWN2)
    tok_wait(5, UP2)
    all_sib(0)
    gate(0)
    begin(5)
    for i in order:
        relay(3, i)
    all_sib(1)
    up(0)
    for i in order:
        finish(2, i)
    for u in (4, 5):
        relay(u, 0)
    all_sib(2)
    gate(1)
    for i in (1, 3, 2):
        spread(4, i)
        spread(5, i)
    for i in order:
        finish(3, i)
    all_sib(3)
    up(1)
    set_sib(0)
    down(0)
    for u in (4, 5):
        finish(u, 0)
    for i in (1, 3):
        for u in (4, 5):
            relay(u, i)
    set_sib(1)
    down(1)
    pass_on(0)
    set_sib(2)
    down(2)
    pass_on(1)
    for u in (4, 5):
        relay(u, 2)
    set_sib(3)
    down(3)
    pass_on(2)
    for i in (1, 3):
        for u in (4, 5):
            finish(u, i)
    pass_on(3)
    set_sib(4)
    down(4)
    down(5)
    pass_on(4)
    down(6)
    for u in (4, 5):
        finish(u, 2)
    pass_on(5)
    pass_on(6)
    set_sib(7)
    down(7)
    for step in range(6):
        total_of(step)
    pass_on(7)
    total_of(6)
    total_of(7)

    for u, (m, p) in enumerate(UNITS):
        landed(W.at[:, 0:5, 0, 0:H, 0:128], w_send.at[u])
        landed(W.at[m, :, p, half_of(c), :], s_send.at[u])
    landed(W.at[:, 0, 0, 0:H, 0:128], x_send)
    landed(T.at[0:6 * HALF], t_send)
    landed(S, q_send)


def layer(tokens, norm_gain, gate_weight, up_weight, down_weight):
    vmem = pl.BlockSpec(memory_space=pltpu.VMEM)
    hbm = pl.BlockSpec(memory_space=pl.ANY)
    dma = pltpu.SemaphoreType.DMA
    return pl.pallas_call(
        kernel,
        out_shape=pltpu.VMEM((ROWS, D), BF16),
        in_specs=[hbm, vmem] + [hbm] * 3,
        out_specs=vmem,
        scratch_shapes=[
            pltpu.VMEM((ROWS, D), BF16),
            pltpu.VMEM((M, D), BF16),
            pltpu.VMEM((3, PAIRS, 2, WIDE, 256), BF16),
            pltpu.VMEM((M, WIDE), F32),
            pltpu.VMEM((2, M, WIDE), BF16),
            pltpu.VMEM((PAIRS, 2 * ROWS, 256), F32),
            pltpu.VMEM((PAIRS, 6, HALF, 256), BF16),
            pltpu.VMEM((PAIRS, 6, HALF, 256), BF16),
            dma((4,)),
            dma((len(UNITS),)), dma((len(UNITS), SLOTS)),
            dma((len(UNITS),)), dma((4 + len(STEPS),)),
            dma, dma((3,)),
            dma, dma((6,)),
            dma, dma((len(STEPS), 3)),
        ],
        compiler_params=pltpu.CompilerParams(
            collective_id=0, has_side_effects=True, vmem_limit_bytes=60 * 1024 * 1024),
    )(tokens, norm_gain.reshape(1, D), gate_weight.T, up_weight.T, down_weight)


def solution(mesh):
    return jax.shard_map(
        layer,
        mesh=mesh,
        in_specs=(P(("fs", "tp"), None), P(), P("fs", "tp"), P("fs", "tp"), P("tp", "fs")),
        out_specs=P(("fs", "tp"), None),
        check_vma=False,
    )
```

```python
import jax
import jax.numpy as jnp
from jax import lax
from jax.experimental import pallas as pl
from jax.experimental.pallas import tpu as pltpu
from jax.sharding import PartitionSpec as P

eps_floor = 0.05
MESH = pl.DeviceIdType.MESH
F32 = jnp.float32
BF16 = jnp.bfloat16

SIDE, Z = 4, 8
ROWS, D, H = 128, 2048, 352
HALF = ROWS // 2
SLOTS = SIDE * SIDE
PAIRS = SLOTS // 2
UNITS = ((0, 0), (1, 0), (0, 1), (1, 1), (2, 0), (2, 1))
OWN, DOWN1, UP1, DOWN2, UP2 = 0, ROWS, 2 * ROWS, 3 * ROWS, 3 * ROWS + HALF
M = 4 * ROWS
FIRST = ((0, -1, DOWN2), (1, -1, DOWN1 + HALF), (3, 1, UP2), (4, 1, UP1))
SECOND = ((2, -1, 0, ROWS), (5, 1, 3, ROWS + HALF))
WIDE = 2 * H
STEPS = ((0, 0), (0, 1), (1, 0), (3, 0), (2, 0), (1, 1), (3, 1), (2, 1))
NEEDS = {0: ((0, 0), (0, 1), (0, 3), (1, 0), (3, 0)), 1: ((0, 2), (2, 0)), 2: ((1, 1), (1, 3), (3, 1)), 3: ((3, 3),),
         4: ((2, 1), (2, 3), (1, 2), (3, 2)), 7: ((2, 2),)}
SET_OF = {piece: step for step, pieces in NEEDS.items() for piece in pieces}
TILES = tuple((n, min(n + 256, WIDE)) for n in range(0, WIDE, 256))


def kernel(tok, gain, gw, uw, dw, out, raw, T, W, G, hid, part, S, R,
           local, w_send, w_recv, s_send, s_recv, x_send, x_recv, t_send, t_recv, q_send, q_recv):
    f, t = lax.axis_index("fs"), lax.axis_index("tp")
    y, x, z, c = f // SIDE, f % SIDE, t // 2, t % 2

    def fs_at(j, i, core=c):
        dy = jnp.where(core == 0, j, i)
        dx = jnp.where(core == 0, i, j)
        return lax.rem(y + dy, SIDE) * SIDE + lax.rem(x + dx, SIDE)

    def z_at(dz):
        return {"tp": lax.rem(z + dz + Z, Z) * 2 + c}

    sib = {"tp": z * 2 + 1 - c}

    barrier = pltpu.get_barrier_semaphore()
    peers = [{"fs": fs_at(j, i)} for j, i in ((0, 1), (0, 3), (1, 0), (3, 0), (0, 2))]
    peers += [z_at(dz) for dz in (1, -1, 4)] + [sib]
    for peer in peers:
        pl.semaphore_signal(barrier, inc=1, device_id=peer, device_id_type=MESH)

    def piece(m, p, fs, core):
        return W.at[m, fs // 2, p, pl.ds(pl.multiple_of(core * H, 32), H),
                    pl.ds(pl.multiple_of((fs % 2) * 128, 128), 128)]

    own = [pltpu.make_async_copy(ref, piece(m, 0, f, c), local.at[m]) for m, ref in enumerate((gw, uw, dw))]
    raw_copy = pltpu.make_async_copy(tok, raw, local.at[3])
    for cp in own:
        cp.start()
    raw_copy.start()
    pl.semaphore_wait(barrier, len(peers))
    for cp in own:
        cp.wait()

    def send(src, dst, send_sem, recv_sem, device):
        cp = pltpu.make_async_remote_copy(src_ref=src, dst_ref=dst, send_sem=send_sem, recv_sem=recv_sem,
                                          device_id=device, device_id_type=MESH)
        cp.start()

    def landed(ref, sem):
        pltpu.make_async_copy(ref, ref, sem).wait()

    def hop(u, j, i, dj, di):
        m, p = UNITS[u]
        ref = piece(m, p, fs_at(j, i), c)
        slot = ((j - dj) % SIDE) * SIDE + (i - di) % SIDE
        send(ref, ref, w_send.at[u], w_recv.at[u, slot], {"fs": fs_at(dj, di)})

    def to_sib(u, j, i):
        m, p = UNITS[u]
        ref = piece(m, p, fs_at(j, i), c)
        k = u if u < 4 else 4 + SET_OF[j, i]
        send(ref, ref, s_send.at[u], s_recv.at[k], sib)

    def half_of(core):
        return pl.ds(pl.multiple_of(core * H, 32), H)

    def all_sib(u):
        m, p = UNITS[u]
        landed(W.at[m, :, p, half_of(1 - c), :], s_recv.at[u])

    def set_sib(step):
        landed(W.at[2, 0:len(NEEDS[step]), :, half_of(1 - c), 0:128], s_recv.at[4 + step])

    def arrive(u, j, i):
        m, p = UNITS[u]
        landed(piece(m, p, fs_at(j, i), c), w_recv.at[u, j * SIDE + i])

    def exchange(m):
        send(piece(m, 0, f, c), piece(m, 1, f, c), x_send, x_recv.at[m], z_at(4))

    def begin(u):
        m, p = UNITS[u]
        if p == 1:
            landed(piece(m, 1, f, c), x_recv.at[m])
        for di in (1, 3, 2):
            hop(u, 0, 0, 0, di)
        for dj in (1, 3):
            hop(u, 0, 0, dj, 0)
        to_sib(u, 0, 0)

    def spread(u, i):
        arrive(u, 0, i)
        hop(u, 0, i, 1, 0)
        hop(u, 0, i, 3, 0)
        to_sib(u, 0, i)

    def relay(u, i):
        for j in ((3, 1) if i % 2 == 0 else (1, 3)):
            arrive(u, j, i)
            if i % 2 == 0 and j == 3:
                hop(u, 3, i, 1, 0)
            if i % 2 == 1 and j == 1:
                hop(u, 1, i, 3, 0)
            to_sib(u, j, i)

    def finish(u, i):
        arrive(u, 2, i)
        to_sib(u, 2, i)

    order = (0, 1, 3, 2)

    def tok_send(k, src, dst, dz):
        send(T.at[src:src + HALF], T.at[dst:dst + HALF], t_send, t_recv.at[k], z_at(dz))

    def tok_wait(k, dst):
        landed(T.at[dst:dst + HALF], t_recv.at[k])

    def wide_dot(m, p, n0, n1):
        total = None
        for q in range(PAIRS):
            d = lax.dot_general(T[:, q * 256:(q + 1) * 256], W[m, q, p, n0:n1, :],
                                (((1,), (1,)), ((), ())), preferred_element_type=F32)
            total = d if total is None else total + d
        return total

    def gate(p):
        for n0, n1 in TILES:
            G[:, n0:n1] = wide_dot(0, p, n0, n1)

    def up(p):
        for n0, n1 in TILES:
            hid[p, :, n0:n1] = (jax.nn.silu(G[:, n0:n1]) * wide_dot(1, p, n0, n1)).astype(BF16)

    def pair_of(step):
        dy, far = STEPS[step]
        px = x // 2
        return lax.rem(y + dy, SIDE) * 2 + (1 - px if far else px)

    def sum_send(step, k, dz):
        q = pair_of(step)
        lot = (0, 2, 2, 1, 2, 2)[k]
        send(S.at[q, k], R.at[q, k], q_send, q_recv.at[step, lot], z_at(dz))

    def down(step):
        q = pair_of(step)
        total = None
        for p in range(2):
            d = jnp.dot(hid[p], W[2, q, p], preferred_element_type=F32)
            total = d if total is None else total + d
        part[q, :ROWS] = total[:ROWS]
        part[q, ROWS:ROWS + HALF] = total[DOWN1:DOWN1 + HALF]
        part[q, ROWS + HALF:] = total[UP1 + HALF:UP1 + ROWS]
        for k, dz, r0 in FIRST:
            S[q, k] = total[r0:r0 + HALF].astype(BF16)
            sum_send(step, k, dz)

    def pass_on(step):
        q = pair_of(step)
        for lot, (k, dz, source, r0) in enumerate(SECOND):
            landed(R.at[q, source], q_recv.at[step, lot])
            S[q, k] = (part[q, r0:r0 + HALF] + R[q, source].astype(F32)).astype(BF16)
            sum_send(step, k, dz)

    def total_of(step):
        q = pair_of(step)
        landed(R.at[q, 0:4], q_recv.at[step, 2])
        for a, first, second in ((0, 4, 2), (HALF, 1, 5)):
            total = part[q, a:a + HALF] + R[q, first].astype(F32) + R[q, second].astype(F32)
            out[a:a + HALF, pl.ds(pl.multiple_of(q * 256, 256), 256)] = total.astype(BF16)

    begin(0)
    exchange(0)
    begin(1)
    exchange(1)
    raw_copy.wait()
    values = raw[...].astype(F32)
    factor = lax.rsqrt(jnp.mean(values * values, axis=-1, keepdims=True) + eps_floor)
    T[OWN:OWN + ROWS] = (values * factor * gain[...]).astype(BF16)
    tok_send(0, OWN, DOWN1, 1)
    tok_send(1, OWN + HALF, UP1 + HALF, -1)
    tok_send(2, OWN + HALF, DOWN1 + HALF, 1)
    tok_send(3, OWN, UP1, -1)
    for i in (1, 3, 2):
        spread(0, i)
    begin(2)
    for i in (1, 3, 2):
        spread(1, i)
    for i in order:
        relay(0, i)
    begin(3)
    for i in (1, 3, 2):
        spread(2, i)
    tok_wait(0, DOWN1)
    tok_send(4, DOWN1, DOWN2, 1)
    tok_wait(1, UP1 + HALF)
    tok_send(5, UP1 + HALF, UP2, -1)
    exchange(2)
    for i in order:
        relay(1, i)
    for i in order:
        finish(0, i)
    for i in (1, 3, 2):
        spread(3, i)
    for i in order:
        relay(2, i)
    for i in order:
        finish(1, i)
    tok_wait(2, DOWN1 + HALF)
    tok_wait(3, UP1)
    tok_wait(4, DOWN2)
    tok_wait(5, UP2)
    all_sib(0)
    gate(0)
    for i in order:
        relay(3, i)
    begin(4)
    begin(5)
    all_sib(1)
    up(0)
    for i in order:
        finish(2, i)
    for u in (4, 5):
        for i in (1, 3):
            spread(u, i)
    all_sib(2)
    gate(1)
    for i in order:
        finish(3, i)
    for u in (4, 5):
        relay(u, 0)
        spread(u, 2)
    all_sib(3)
    up(1)
    set_sib(0)
    down(0)
    for u in (4, 5):
        finish(u, 0)
    for u in (4, 5):
        relay(u, 1)
    set_sib(1)
    down(1)
    for u in (4, 5):
        relay(u, 3)
    set_sib(2)
    down(2)
    pass_on(0)
    set_sib(3)
    down(3)
    for u in (4, 5):
        relay(u, 2)
    pass_on(1)
    for i in (1, 3):
        for u in (4, 5):
            finish(u, i)
    pass_on(2)
    set_sib(4)
    down(4)
    pass_on(3)
    down(5)
    down(6)
    for u in (4, 5):
        finish(u, 2)
    set_sib(7)
    down(7)
    for step in (4, 5, 6):
        pass_on(step)
    for step in range(4):
        total_of(step)
    pass_on(7)
    for step in range(4, len(STEPS)):
        total_of(step)

    for u, (m, p) in enumerate(UNITS):
        landed(W.at[:, 0:5, 0, 0:H, 0:128], w_send.at[u])
        landed(W.at[m, :, p, half_of(c), :], s_send.at[u])
    landed(W.at[:, 0, 0, 0:H, 0:128], x_send)
    landed(T.at[0:6 * HALF], t_send)
    landed(S, q_send)


def layer(tokens, norm_gain, gate_weight, up_weight, down_weight):
    vmem = pl.BlockSpec(memory_space=pltpu.VMEM)
    hbm = pl.BlockSpec(memory_space=pl.ANY)
    dma = pltpu.SemaphoreType.DMA
    return pl.pallas_call(
        kernel,
        out_shape=pltpu.VMEM((ROWS, D), BF16),
        in_specs=[hbm, vmem] + [hbm] * 3,
        out_specs=vmem,
        scratch_shapes=[
            pltpu.VMEM((ROWS, D), BF16),
            pltpu.VMEM((M, D), BF16),
            pltpu.VMEM((3, PAIRS, 2, WIDE, 256), BF16),
            pltpu.VMEM((M, WIDE), F32),
            pltpu.VMEM((2, M, WIDE), BF16),
            pltpu.VMEM((PAIRS, 2 * ROWS, 256), F32),
            pltpu.VMEM((PAIRS, 6, HALF, 256), BF16),
            pltpu.VMEM((PAIRS, 6, HALF, 256), BF16),
            dma((4,)),
            dma((len(UNITS),)), dma((len(UNITS), SLOTS)),
            dma((len(UNITS),)), dma((4 + len(STEPS),)),
            dma, dma((3,)),
            dma, dma((6,)),
            dma, dma((len(STEPS), 3)),
        ],
        compiler_params=pltpu.CompilerParams(
            collective_id=0, has_side_effects=True, vmem_limit_bytes=60 * 1024 * 1024),
    )(tokens, norm_gain.reshape(1, D), gate_weight.T, up_weight.T, down_weight)


def solution(mesh):
    return jax.shard_map(
        layer,
        mesh=mesh,
        in_specs=(P(("fs", "tp"), None), P(), P("fs", "tp"), P("fs", "tp"), P("tp", "fs")),
        out_specs=P(("fs", "tp"), None),
        check_vma=False,
    )
```

```python
import jax
import jax.numpy as jnp
from jax import lax
from jax.experimental import pallas as pl
from jax.experimental.pallas import tpu as pltpu
from jax.sharding import PartitionSpec as P

eps_floor = 0.05
MESH = pl.DeviceIdType.MESH
F32 = jnp.float32
BF16 = jnp.bfloat16

SIDE, Z = 4, 8
ROWS, D, H = 128, 2048, 352
HALF = ROWS // 2
SLOTS = SIDE * SIDE
PAIRS = SLOTS // 2
UNITS = ((0, 0), (1, 0), (0, 1), (1, 1), (2, 0), (2, 1))
OWN, DOWN1, UP1, DOWN2, UP2 = 0, ROWS, 2 * ROWS, 3 * ROWS, 3 * ROWS + HALF
M = 4 * ROWS
FIRST = ((0, -1, DOWN2), (1, -1, DOWN1 + HALF), (3, 1, UP2), (4, 1, UP1))
SECOND = ((2, -1, 0, ROWS), (5, 1, 3, ROWS + HALF))
WIDE = 2 * H
STEPS = ((0, 0), (0, 1), (1, 0), (3, 0), (2, 0), (1, 1), (3, 1), (2, 1))
NEEDS = {0: ((0, 0), (0, 1), (0, 3), (1, 0), (3, 0)), 1: ((0, 2), (2, 0)), 2: ((1, 1), (1, 3), (3, 1)), 3: ((3, 3),),
         4: ((2, 1), (2, 3), (1, 2), (3, 2)), 7: ((2, 2),)}
SET_OF = {piece: step for step, pieces in NEEDS.items() for piece in pieces}
TILES = tuple((n, min(n + 256, WIDE)) for n in range(0, WIDE, 256))


def kernel(tok, gain, gw, uw, dw, out, raw, T, W, G, hid, part, S, R,
           local, w_send, w_recv, s_send, s_recv, x_send, x_recv, t_send, t_recv, q_send, q_recv):
    f, t = lax.axis_index("fs"), lax.axis_index("tp")
    y, x, z, c = f // SIDE, f % SIDE, t // 2, t % 2

    def fs_at(j, i, core=c):
        dy = jnp.where(core == 0, j, i)
        dx = jnp.where(core == 0, i, j)
        return lax.rem(y + dy, SIDE) * SIDE + lax.rem(x + dx, SIDE)

    def z_at(dz):
        return {"tp": lax.rem(z + dz + Z, Z) * 2 + c}

    sib = {"tp": z * 2 + 1 - c}

    barrier = pltpu.get_barrier_semaphore()
    peers = [{"fs": fs_at(j, i)} for j, i in ((0, 1), (0, 3), (1, 0), (3, 0), (0, 2))]
    peers += [z_at(dz) for dz in (1, -1, 4)] + [sib]
    for peer in peers:
        pl.semaphore_signal(barrier, inc=1, device_id=peer, device_id_type=MESH)

    def piece(m, p, fs, core):
        return W.at[m, fs // 2, p, pl.ds(pl.multiple_of(core * H, 32), H),
                    pl.ds(pl.multiple_of((fs % 2) * 128, 128), 128)]

    own = [pltpu.make_async_copy(ref, piece(m, 0, f, c), local.at[m]) for m, ref in enumerate((gw, uw, dw))]
    raw_copy = pltpu.make_async_copy(tok, raw, local.at[3])
    for cp in own:
        cp.start()
    raw_copy.start()
    pl.semaphore_wait(barrier, len(peers))
    for cp in own:
        cp.wait()

    def send(src, dst, send_sem, recv_sem, device):
        cp = pltpu.make_async_remote_copy(src_ref=src, dst_ref=dst, send_sem=send_sem, recv_sem=recv_sem,
                                          device_id=device, device_id_type=MESH)
        cp.start()

    def landed(ref, sem):
        pltpu.make_async_copy(ref, ref, sem).wait()

    def hop(u, j, i, dj, di):
        m, p = UNITS[u]
        ref = piece(m, p, fs_at(j, i), c)
        slot = ((j - dj) % SIDE) * SIDE + (i - di) % SIDE
        send(ref, ref, w_send.at[u], w_recv.at[u, slot], {"fs": fs_at(dj, di)})

    def to_sib(u, j, i):
        m, p = UNITS[u]
        ref = piece(m, p, fs_at(j, i), c)
        k = u if u < 4 else 4 + SET_OF[j, i]
        send(ref, ref, s_send.at[u], s_recv.at[k], sib)

    def half_of(core):
        return pl.ds(pl.multiple_of(core * H, 32), H)

    def all_sib(u):
        m, p = UNITS[u]
        landed(W.at[m, :, p, half_of(1 - c), :], s_recv.at[u])

    def set_sib(step):
        landed(W.at[2, 0:len(NEEDS[step]), :, half_of(1 - c), 0:128], s_recv.at[4 + step])

    def arrive(u, j, i):
        m, p = UNITS[u]
        landed(piece(m, p, fs_at(j, i), c), w_recv.at[u, j * SIDE + i])

    def exchange(m):
        send(piece(m, 0, f, c), piece(m, 1, f, c), x_send, x_recv.at[m], z_at(4))

    def begin(u):
        m, p = UNITS[u]
        if p == 1:
            landed(piece(m, 1, f, c), x_recv.at[m])
        for di in (1, 3, 2):
            hop(u, 0, 0, 0, di)
        for dj in (1, 3):
            hop(u, 0, 0, dj, 0)
        to_sib(u, 0, 0)

    def spread(u, i):
        arrive(u, 0, i)
        hop(u, 0, i, 1, 0)
        hop(u, 0, i, 3, 0)
        to_sib(u, 0, i)

    def relay(u, i):
        for j in ((3, 1) if i % 2 == 0 else (1, 3)):
            arrive(u, j, i)
            if i % 2 == 0 and j == 3:
                hop(u, 3, i, 1, 0)
            if i % 2 == 1 and j == 1:
                hop(u, 1, i, 3, 0)
            to_sib(u, j, i)

    def finish(u, i):
        arrive(u, 2, i)
        to_sib(u, 2, i)

    order = (0, 1, 3, 2)

    def tok_send(k, src, dst, dz):
        send(T.at[src:src + HALF], T.at[dst:dst + HALF], t_send, t_recv.at[k], z_at(dz))

    def tok_wait(k, dst):
        landed(T.at[dst:dst + HALF], t_recv.at[k])

    def wide_dot(m, p, n0, n1):
        total = None
        for q in range(PAIRS):
            d = lax.dot_general(T[:, q * 256:(q + 1) * 256], W[m, q, p, n0:n1, :],
                                (((1,), (1,)), ((), ())), preferred_element_type=F32)
            total = d if total is None else total + d
        return total

    def gate(p):
        for n0, n1 in TILES:
            G[:, n0:n1] = wide_dot(0, p, n0, n1)

    def up(p):
        for n0, n1 in TILES:
            hid[p, :, n0:n1] = (jax.nn.silu(G[:, n0:n1]) * wide_dot(1, p, n0, n1)).astype(BF16)

    def pair_of(step):
        dy, far = STEPS[step]
        px = x // 2
        return lax.rem(y + dy, SIDE) * 2 + (1 - px if far else px)

    def sum_send(step, k, dz):
        q = pair_of(step)
        lot = (0, 2, 2, 1, 2, 2)[k]
        send(S.at[q, k], R.at[q, k], q_send, q_recv.at[step, lot], z_at(dz))

    def down(step):
        q = pair_of(step)
        total = None
        for p in range(2):
            d = jnp.dot(hid[p], W[2, q, p], preferred_element_type=F32)
            total = d if total is None else total + d
        part[q, :ROWS] = total[:ROWS]
        part[q, ROWS:ROWS + HALF] = total[DOWN1:DOWN1 + HALF]
        part[q, ROWS + HALF:] = total[UP1 + HALF:UP1 + ROWS]
        for k, dz, r0 in FIRST:
            S[q, k] = total[r0:r0 + HALF].astype(BF16)
            sum_send(step, k, dz)

    def pass_on(step):
        q = pair_of(step)
        for lot, (k, dz, source, r0) in enumerate(SECOND):
            landed(R.at[q, source], q_recv.at[step, lot])
            S[q, k] = (part[q, r0:r0 + HALF] + R[q, source].astype(F32)).astype(BF16)
            sum_send(step, k, dz)

    def total_of(step):
        q = pair_of(step)
        landed(R.at[q, 0:4], q_recv.at[step, 2])
        for a, first, second in ((0, 4, 2), (HALF, 1, 5)):
            total = part[q, a:a + HALF] + R[q, first].astype(F32) + R[q, second].astype(F32)
            out[a:a + HALF, pl.ds(pl.multiple_of(q * 256, 256), 256)] = total.astype(BF16)

    begin(0)
    exchange(0)
    begin(1)
    exchange(1)
    raw_copy.wait()
    values = raw[...].astype(F32)
    factor = lax.rsqrt(jnp.mean(values * values, axis=-1, keepdims=True) + eps_floor)
    T[OWN:OWN + ROWS] = (values * factor * gain[...]).astype(BF16)
    tok_send(0, OWN, DOWN1, 1)
    tok_send(1, OWN + HALF, UP1 + HALF, -1)
    tok_send(2, OWN + HALF, DOWN1 + HALF, 1)
    tok_send(3, OWN, UP1, -1)
    for i in (1, 3, 2):
        spread(0, i)
    begin(2)
    for i in (1, 3, 2):
        spread(1, i)
    for i in order:
        relay(0, i)
    begin(3)
    for i in (1, 3, 2):
        spread(2, i)
    tok_wait(0, DOWN1)
    tok_send(4, DOWN1, DOWN2, 1)
    tok_wait(1, UP1 + HALF)
    tok_send(5, UP1 + HALF, UP2, -1)
    exchange(2)
    for i in order:
        relay(1, i)
    for i in order:
        finish(0, i)
    for i in (1, 3, 2):
        spread(3, i)
    for i in order:
        relay(2, i)
    for i in order:
        finish(1, i)
    for i in order:
        relay(3, i)
    begin(4)
    begin(5)
    tok_wait(2, DOWN1 + HALF)
    tok_wait(3, UP1)
    tok_wait(4, DOWN2)
    tok_wait(5, UP2)
    all_sib(0)
    gate(0)
    all_sib(1)
    up(0)
    for i in order:
        finish(2, i)
    for u in (4, 5):
        for i in (1, 3):
            spread(u, i)
    all_sib(2)
    gate(1)
    for i in order:
        finish(3, i)
    for u in (4, 5):
        relay(u, 0)
        spread(u, 2)
    all_sib(3)
    for u in (4, 5):
        relay(u, 1)
    up(1)
    set_sib(0)
    down(0)
    for u in (4, 5):
        relay(u, 3)
    for u in (4, 5):
        finish(u, 0)
    set_sib(1)
    down(1)
    for u in (4, 5):
        relay(u, 2)
    set_sib(2)
    down(2)
    pass_on(0)
    set_sib(3)
    down(3)
    pass_on(1)
    for i in (1, 3):
        for u in (4, 5):
            finish(u, i)
    pass_on(2)
    set_sib(4)
    down(4)
    pass_on(3)
    down(5)
    down(6)
    for u in (4, 5):
        finish(u, 2)
    set_sib(7)
    down(7)
    for step in (4, 5, 6):
        pass_on(step)
    for step in range(4):
        total_of(step)
    pass_on(7)
    for step in range(4, len(STEPS)):
        total_of(step)

    for u, (m, p) in enumerate(UNITS):
        landed(W.at[:, 0:5, 0, 0:H, 0:128], w_send.at[u])
        landed(W.at[m, :, p, half_of(c), :], s_send.at[u])
    landed(W.at[:, 0, 0, 0:H, 0:128], x_send)
    landed(T.at[0:6 * HALF], t_send)
    landed(S, q_send)


def layer(tokens, norm_gain, gate_weight, up_weight, down_weight):
    vmem = pl.BlockSpec(memory_space=pltpu.VMEM)
    hbm = pl.BlockSpec(memory_space=pl.ANY)
    dma = pltpu.SemaphoreType.DMA
    return pl.pallas_call(
        kernel,
        out_shape=pltpu.VMEM((ROWS, D), BF16),
        in_specs=[hbm, vmem] + [hbm] * 3,
        out_specs=vmem,
        scratch_shapes=[
            pltpu.VMEM((ROWS, D), BF16),
            pltpu.VMEM((M, D), BF16),
            pltpu.VMEM((3, PAIRS, 2, WIDE, 256), BF16),
            pltpu.VMEM((M, WIDE), F32),
            pltpu.VMEM((2, M, WIDE), BF16),
            pltpu.VMEM((PAIRS, 2 * ROWS, 256), F32),
            pltpu.VMEM((PAIRS, 6, HALF, 256), BF16),
            pltpu.VMEM((PAIRS, 6, HALF, 256), BF16),
            dma((4,)),
            dma((len(UNITS),)), dma((len(UNITS), SLOTS)),
            dma((len(UNITS),)), dma((4 + len(STEPS),)),
            dma, dma((3,)),
            dma, dma((6,)),
            dma, dma((len(STEPS), 3)),
        ],
        compiler_params=pltpu.CompilerParams(
            collective_id=0, has_side_effects=True, vmem_limit_bytes=60 * 1024 * 1024),
    )(tokens, norm_gain.reshape(1, D), gate_weight.T, up_weight.T, down_weight)


def solution(mesh):
    return jax.shard_map(
        layer,
        mesh=mesh,
        in_specs=(P(("fs", "tp"), None), P(), P("fs", "tp"), P("fs", "tp"), P("tp", "fs")),
        out_specs=P(("fs", "tp"), None),
        check_vma=False,
    )
```

```python
import jax
import jax.numpy as jnp
from jax import lax
from jax.experimental import pallas as pl
from jax.experimental.pallas import tpu as pltpu
from jax.sharding import PartitionSpec as P

eps_floor = 0.05
MESH = pl.DeviceIdType.MESH
F32 = jnp.float32
BF16 = jnp.bfloat16

SIDE, Z = 4, 8
ROWS, D, H = 128, 2048, 352
HALF = ROWS // 2
SLOTS = SIDE * SIDE
PAIRS = SLOTS // 2
UNITS = ((0, 0), (1, 0), (0, 1), (1, 1), (2, 0), (2, 1))
OWN, DOWN1, UP1, DOWN2, UP2 = 0, ROWS, 2 * ROWS, 3 * ROWS, 3 * ROWS + HALF
M = 4 * ROWS
FIRST = ((0, -1, DOWN2), (1, -1, DOWN1 + HALF), (3, 1, UP2), (4, 1, UP1))
SECOND = ((2, -1, 0, ROWS), (5, 1, 3, ROWS + HALF))
WIDE = 2 * H
STEPS = ((0, 0), (0, 1), (1, 0), (3, 0), (2, 0), (1, 1), (3, 1), (2, 1))
NEEDS = {0: ((0, 0), (0, 1), (0, 3), (1, 0), (3, 0)), 1: ((0, 2), (2, 0)), 2: ((1, 1), (1, 3), (3, 1)), 3: ((3, 3),),
         4: ((2, 1), (2, 3), (1, 2), (3, 2)), 7: ((2, 2),)}
SET_OF = {piece: step for step, pieces in NEEDS.items() for piece in pieces}
TILES = tuple((n, min(n + 256, WIDE)) for n in range(0, WIDE, 256))


def kernel(tok, gain, gw, uw, dw, out, raw, T, W, G, hid, part, S, R,
           local, w_send, w_recv, s_send, s_recv, x_send, x_recv, t_send, t_recv, q_send, q_recv):
    f, t = lax.axis_index("fs"), lax.axis_index("tp")
    y, x, z, c = f // SIDE, f % SIDE, t // 2, t % 2

    def fs_at(j, i, core=c):
        dy = jnp.where(core == 0, j, i)
        dx = jnp.where(core == 0, i, j)
        return lax.rem(y + dy, SIDE) * SIDE + lax.rem(x + dx, SIDE)

    def z_at(dz):
        return {"tp": lax.rem(z + dz + Z, Z) * 2 + c}

    sib = {"tp": z * 2 + 1 - c}

    barrier = pltpu.get_barrier_semaphore()
    peers = [{"fs": fs_at(j, i)} for j, i in ((0, 1), (0, 3), (1, 0), (3, 0), (0, 2))]
    peers += [z_at(dz) for dz in (1, -1, 4)] + [sib]
    for peer in peers:
        pl.semaphore_signal(barrier, inc=1, device_id=peer, device_id_type=MESH)

    def piece(m, p, fs, core):
        return W.at[m, fs // 2, p, pl.ds(pl.multiple_of(core * H, 32), H),
                    pl.ds(pl.multiple_of((fs % 2) * 128, 128), 128)]

    own = [pltpu.make_async_copy(ref, piece(m, 0, f, c), local.at[m]) for m, ref in enumerate((gw, uw, dw))]
    raw_copy = pltpu.make_async_copy(tok, raw, local.at[3])
    for cp in own:
        cp.start()
    raw_copy.start()
    pl.semaphore_wait(barrier, len(peers))
    for cp in own:
        cp.wait()

    def send(src, dst, send_sem, recv_sem, device):
        cp = pltpu.make_async_remote_copy(src_ref=src, dst_ref=dst, send_sem=send_sem, recv_sem=recv_sem,
                                          device_id=device, device_id_type=MESH)
        cp.start()

    def landed(ref, sem):
        pltpu.make_async_copy(ref, ref, sem).wait()

    def hop(u, j, i, dj, di):
        m, p = UNITS[u]
        ref = piece(m, p, fs_at(j, i), c)
        slot = ((j - dj) % SIDE) * SIDE + (i - di) % SIDE
        send(ref, ref, w_send.at[u], w_recv.at[u, slot], {"fs": fs_at(dj, di)})

    def to_sib(u, j, i):
        m, p = UNITS[u]
        ref = piece(m, p, fs_at(j, i), c)
        k = u if u < 4 else 4 + SET_OF[j, i]
        send(ref, ref, s_send.at[u], s_recv.at[k], sib)

    def half_of(core):
        return pl.ds(pl.multiple_of(core * H, 32), H)

    def all_sib(u):
        m, p = UNITS[u]
        landed(W.at[m, :, p, half_of(1 - c), :], s_recv.at[u])

    def set_sib(step):
        landed(W.at[2, 0:len(NEEDS[step]), :, half_of(1 - c), 0:128], s_recv.at[4 + step])

    def arrive(u, j, i):
        m, p = UNITS[u]
        landed(piece(m, p, fs_at(j, i), c), w_recv.at[u, j * SIDE + i])

    def exchange(m):
        send(piece(m, 0, f, c), piece(m, 1, f, c), x_send, x_recv.at[m], z_at(4))

    def begin(u):
        m, p = UNITS[u]
        if p == 1:
            landed(piece(m, 1, f, c), x_recv.at[m])
        for di in (1, 3, 2):
            hop(u, 0, 0, 0, di)
        for dj in (1, 3):
            hop(u, 0, 0, dj, 0)
        to_sib(u, 0, 0)

    def spread(u, i):
        arrive(u, 0, i)
        hop(u, 0, i, 1, 0)
        hop(u, 0, i, 3, 0)
        to_sib(u, 0, i)

    def relay(u, i):
        for j in ((3, 1) if i % 2 == 0 else (1, 3)):
            arrive(u, j, i)
            if i % 2 == 0 and j == 3:
                hop(u, 3, i, 1, 0)
            if i % 2 == 1 and j == 1:
                hop(u, 1, i, 3, 0)
            to_sib(u, j, i)

    def finish(u, i):
        arrive(u, 2, i)
        to_sib(u, 2, i)

    order = (0, 1, 3, 2)

    def tok_send(k, src, dst, dz):
        send(T.at[src:src + HALF], T.at[dst:dst + HALF], t_send, t_recv.at[k], z_at(dz))

    def tok_wait(k, dst):
        landed(T.at[dst:dst + HALF], t_recv.at[k])

    def wide_dot(m, p, n0, n1):
        total = None
        for q in range(PAIRS):
            d = lax.dot_general(T[:, q * 256:(q + 1) * 256], W[m, q, p, n0:n1, :],
                                (((1,), (1,)), ((), ())), preferred_element_type=F32)
            total = d if total is None else total + d
        return total

    def gate(p):
        for n0, n1 in TILES:
            G[:, n0:n1] = wide_dot(0, p, n0, n1)

    def up(p):
        for n0, n1 in TILES:
            hid[p, :, n0:n1] = (jax.nn.silu(G[:, n0:n1]) * wide_dot(1, p, n0, n1)).astype(BF16)

    def pair_of(step):
        dy, far = STEPS[step]
        px = x // 2
        return lax.rem(y + dy, SIDE) * 2 + (1 - px if far else px)

    def sum_send(step, k, dz):
        q = pair_of(step)
        lot = (0, 2, 2, 1, 2, 2)[k]
        send(S.at[q, k], R.at[q, k], q_send, q_recv.at[step, lot], z_at(dz))

    def down(step):
        q = pair_of(step)
        total = None
        for p in range(2):
            d = jnp.dot(hid[p], W[2, q, p], preferred_element_type=F32)
            total = d if total is None else total + d
        part[q, :ROWS] = total[:ROWS]
        part[q, ROWS:ROWS + HALF] = total[DOWN1:DOWN1 + HALF]
        part[q, ROWS + HALF:] = total[UP1 + HALF:UP1 + ROWS]
        for k, dz, r0 in FIRST:
            S[q, k] = total[r0:r0 + HALF].astype(BF16)
            sum_send(step, k, dz)

    def pass_on(step):
        q = pair_of(step)
        for lot, (k, dz, source, r0) in enumerate(SECOND):
            landed(R.at[q, source], q_recv.at[step, lot])
            S[q, k] = (part[q, r0:r0 + HALF] + R[q, source].astype(F32)).astype(BF16)
            sum_send(step, k, dz)

    def total_of(step):
        q = pair_of(step)
        landed(R.at[q, 0:4], q_recv.at[step, 2])
        for a, first, second in ((0, 4, 2), (HALF, 1, 5)):
            total = part[q, a:a + HALF] + R[q, first].astype(F32) + R[q, second].astype(F32)
            out[a:a + HALF, pl.ds(pl.multiple_of(q * 256, 256), 256)] = total.astype(BF16)

    begin(0)
    exchange(0)
    begin(1)
    exchange(1)
    raw_copy.wait()
    values = raw[...].astype(F32)
    factor = lax.rsqrt(jnp.mean(values * values, axis=-1, keepdims=True) + eps_floor)
    T[OWN:OWN + ROWS] = (values * factor * gain[...]).astype(BF16)
    tok_send(0, OWN, DOWN1, 1)
    tok_send(1, OWN + HALF, UP1 + HALF, -1)
    tok_send(2, OWN + HALF, DOWN1 + HALF, 1)
    tok_send(3, OWN, UP1, -1)
    for i in (1, 3, 2):
        spread(0, i)
    begin(2)
    for i in (1, 3, 2):
        spread(1, i)
    for i in order:
        relay(0, i)
    begin(3)
    for i in (1, 3, 2):
        spread(2, i)
    tok_wait(0, DOWN1)
    tok_send(4, DOWN1, DOWN2, 1)
    tok_wait(1, UP1 + HALF)
    tok_send(5, UP1 + HALF, UP2, -1)
    exchange(2)
    for i in order:
        relay(1, i)
    for i in order:
        finish(0, i)
    for i in (1, 3, 2):
        spread(3, i)
    for i in order:
        relay(2, i)
    for i in order:
        finish(1, i)
    for i in order:
        relay(3, i)
    begin(4)
    begin(5)
    tok_wait(2, DOWN1 + HALF)
    tok_wait(3, UP1)
    tok_wait(4, DOWN2)
    tok_wait(5, UP2)
    all_sib(0)
    gate(0)
    for u in (4, 5):
        for i in (1, 3):
            spread(u, i)
    all_sib(1)
    up(0)
    for i in order:
        finish(2, i)
    all_sib(2)
    gate(1)
    for i in order:
        finish(3, i)
    for u in (4, 5):
        relay(u, 0)
        spread(u, 2)
    all_sib(3)
    for u in (4, 5):
        relay(u, 1)
    up(1)
    set_sib(0)
    down(0)
    for u in (4, 5):
        relay(u, 3)
    for u in (4, 5):
        finish(u, 0)
    set_sib(1)
    down(1)
    for u in (4, 5):
        relay(u, 2)
    set_sib(2)
    down(2)
    pass_on(0)
    set_sib(3)
    down(3)
    pass_on(1)
    for i in (1, 3):
        for u in (4, 5):
            finish(u, i)
    pass_on(2)
    set_sib(4)
    down(4)
    pass_on(3)
    down(5)
    down(6)
    for u in (4, 5):
        finish(u, 2)
    set_sib(7)
    down(7)
    for step in (4, 5, 6):
        pass_on(step)
    for step in range(4):
        total_of(step)
    pass_on(7)
    for step in range(4, len(STEPS)):
        total_of(step)

    for u, (m, p) in enumerate(UNITS):
        landed(W.at[:, 0:5, 0, 0:H, 0:128], w_send.at[u])
        landed(W.at[m, :, p, half_of(c), :], s_send.at[u])
    landed(W.at[:, 0, 0, 0:H, 0:128], x_send)
    landed(T.at[0:6 * HALF], t_send)
    landed(S, q_send)


def layer(tokens, norm_gain, gate_weight, up_weight, down_weight):
    vmem = pl.BlockSpec(memory_space=pltpu.VMEM)
    hbm = pl.BlockSpec(memory_space=pl.ANY)
    dma = pltpu.SemaphoreType.DMA
    return pl.pallas_call(
        kernel,
        out_shape=pltpu.VMEM((ROWS, D), BF16),
        in_specs=[hbm, vmem] + [hbm] * 3,
        out_specs=vmem,
        scratch_shapes=[
            pltpu.VMEM((ROWS, D), BF16),
            pltpu.VMEM((M, D), BF16),
            pltpu.VMEM((3, PAIRS, 2, WIDE, 256), BF16),
            pltpu.VMEM((M, WIDE), F32),
            pltpu.VMEM((2, M, WIDE), BF16),
            pltpu.VMEM((PAIRS, 2 * ROWS, 256), F32),
            pltpu.VMEM((PAIRS, 6, HALF, 256), BF16),
            pltpu.VMEM((PAIRS, 6, HALF, 256), BF16),
            dma((4,)),
            dma((len(UNITS),)), dma((len(UNITS), SLOTS)),
            dma((len(UNITS),)), dma((4 + len(STEPS),)),
            dma, dma((3,)),
            dma, dma((6,)),
            dma, dma((len(STEPS), 3)),
        ],
        compiler_params=pltpu.CompilerParams(
            collective_id=0, has_side_effects=True, vmem_limit_bytes=60 * 1024 * 1024),
    )(tokens, norm_gain.reshape(1, D), gate_weight.T, up_weight.T, down_weight)


def solution(mesh):
    return jax.shard_map(
        layer,
        mesh=mesh,
        in_specs=(P(("fs", "tp"), None), P(), P("fs", "tp"), P("fs", "tp"), P("tp", "fs")),
        out_specs=P(("fs", "tp"), None),
        check_vma=False,
    )
```
